32 devices in a mesh: sp: 8 (over z, core), tp: 4 (over y, x).
Axes of the slice: x: 2, y: 2, z: 4, core: 2. Of those that a mesh axis runs over, the one named last changes fastest.
Arguments:
- query_proj: bfloat16 [2048, 2048], P('sp', 'tp'), may hold values from -4 to 4
- key_proj: bfloat16 [2048, 1024], P('sp', 'tp'), may hold values from -4 to 4
- value_proj: bfloat16 [2048, 1024], P('sp', 'tp'), may hold values from -48 to 48
- query_gain: float32 [32, 64], P('tp'), may hold values from 1 to 6
- key_gain: float32 [16, 64], P('tp'), may hold values from 1 to 6
- residual: bfloat16 [2048, 2048], P('sp', 'tp'), may hold values from -48 to 48
- out_weight: bfloat16 [2048, 2048], P(None, 'tp'), may hold values from -0.125 to 0.125
- route_expert: int32 [2048, 8], P('sp'), may hold values from 0 to 15, all different within a row; in each aligned block of 256 rows (0 to 255, 256 to 511, ...) at most 192 rows name the same one
- route_weight: float32 [2048, 8], P('sp'), may hold values from 0.25 to 1.25
- expert_gate: bfloat16 [32, 2048, 256], P(('sp', 'tp')), may hold values from -0.125 to 0.125
- expert_up: bfloat16 [32, 2048, 256], P(('sp', 'tp')), may hold values from -0.125 to 0.125
- expert_down: bfloat16 [32, 256, 2048], P(('sp', 'tp')), may hold values from -0.25 to 0.25
Outputs:
- block_out: bfloat16 [2048, 2048], P('sp', 'tp')
The draws below stay inside these ranges and needn't reach their ends.
Inputs may be any that keep to these rules, and one draw needn't show every extreme that they name: `route_expert`: A row names 8 different experts; among the rows of one index of sp no expert is named by more than 192 rows, a bound that some block reaches of them.
All inputs are finite; a program needn't handle non-finite values.
Results may differ from the reference program's by a relative error of at most 0.012.
The reference program's roundings to bfloat16 on the way count: a program that leaves them out, or rounds other values in their place, can miss the bound.
Values may be sent and summed in bfloat16 or wider, within the bound.
A program may use at most 64 MiB of HBM per device.

```python
import math
import jax
import jax.numpy as jnp
import numpy as np
from jax import lax

D = 2048
HEADS = 32
KV_HEADS = 16
HEAD_DIM = 64
FF = 512
TOP_K = 8
GRID_W = 64
TOK_DEV = 256
TOKENS = 2048
EXPERTS = 16
CAP = 192
N_SP = 8


def attention_pair(key):
    seeded = jax.random.fold_in(key, 11)
    first_key, second_key = jax.random.split(seeded, 2)
    key_rows = jnp.clip(jax.random.normal(first_key, (TOKENS, KV_HEADS, HEAD_DIM), jnp.float32), -4.0, 4.0)
    query_rows = jnp.clip(jax.random.normal(second_key, (TOKENS, HEADS, HEAD_DIM), jnp.float32), -4.0, 4.0)
    return (query_rows.reshape(TOKENS, HEADS * HEAD_DIM), key_rows.reshape(TOKENS, KV_HEADS * HEAD_DIM))


def draw_query_proj(key, part):
    return attention_pair(key)[0].astype(jnp.bfloat16)


def draw_key_proj(key, part):
    return attention_pair(key)[1].astype(jnp.bfloat16)


def draw_query_gain(key, part):
    seeded = jax.random.fold_in(key, 31)
    return jnp.exp(jax.random.uniform(seeded, (HEADS, HEAD_DIM), jnp.float32, 0.0, 0.6931))


def draw_key_gain(key, part):
    seeded = jax.random.fold_in(key, 37)
    return jnp.exp(jax.random.uniform(seeded, (KV_HEADS, HEAD_DIM), jnp.float32, 0.0, 0.6931))


def draw_residual(key, part):
    seeded = jax.random.fold_in(key, 41)
    first_key, second_key = jax.random.split(seeded, 2)
    fraction = jnp.arange(D, dtype=jnp.float32) / D
    row_scale = jnp.exp(jax.random.uniform(second_key, (TOKENS, 1), jnp.float32, -0.6931, 1.6094))
    column_scale = 0.6 * 3.0 ** fraction
    pattern = jnp.clip(jax.random.normal(first_key, (TOKENS, D), jnp.float32), -4.0, 4.0)
    return (pattern * row_scale * column_scale[None, :]).astype(jnp.bfloat16)


def block_scale(rng, extent, pieces, low, top_value):
    def one(dim, shards_of):
        steps = jax.random.uniform(jax.random.fold_in(jax.random.fold_in(rng, 6), dim), (shards_of,), jnp.float32, low / len(pieces), top_value / len(pieces))
        return jnp.repeat(jnp.exp(steps), extent[dim] // shards_of).reshape((-1,) + (1,) * (len(extent) - dim - 1))

    factor_of = one(*pieces[0])
    for cut in pieces[1:]:
        factor_of = factor_of * one(*cut)
    return factor_of


def assign_block(key, own, number, rows, amount, top, most, skew):
    ranking = jax.random.permutation(key, amount)
    crowded, usual = shares(amount, rows * top, most, skew, True), shares(amount, rows * top, most, skew, False)
    places = jnp.arange(amount)

    def named(sizes, turn):
        used = int((sizes > 0).sum())
        fixed = max(1, used // 4)
        passed = fixed + (places - fixed + turn * (used - fixed)) % max(1, amount - fixed)
        return jnp.zeros((amount,), jnp.int32).at[ranking[jnp.where(places < fixed, places, passed)]].set(jnp.asarray(sizes, jnp.int32))

    sizes = jnp.where(number % 4 == 0, named(crowded, number // 4), named(usual, number - number // 4 - 1))
    mixed = jax.random.permutation(jax.random.fold_in(own, 3), amount)
    giver, receiver = mixed[0:amount // 2 * 2:2], mixed[1:amount // 2 * 2:2]
    margin = jnp.minimum(sizes[giver] - 1, most - sizes[receiver]) // 2
    margin = jnp.where((giver == ranking[0]) | (receiver == ranking[0]) | (sizes[receiver] == 0), 0, jnp.maximum(margin, 0))
    passed = jax.random.randint(jax.random.fold_in(own, 4), (amount // 2,), 0, 1 << 20) % (margin + 1)
    sizes = sizes.at[giver].add(-passed).at[receiver].add(passed)
    labels = jnp.searchsorted(jnp.cumsum(sizes), jnp.arange(rows * top), side="right").astype(jnp.int32)
    grid = labels.reshape(top, rows).T
    grid = grid[jax.random.permutation(jax.random.fold_in(own, 1), rows)]
    turn = jax.random.randint(jax.random.fold_in(own, 2), (rows, 1), 0, top)
    return jnp.take_along_axis(grid, (jnp.arange(top)[None, :] + turn) % top, axis=1)


def shares(count, total, limit, skew, full):
    weights = [(1 << 20) // math.isqrt(grade ** skew) + 1 for grade in range(1, count + 1)]
    largest = limit if full else min(limit, max(-(-total // count), total * weights[0] // sum(weights)))
    least = 1 if total - largest >= count - 1 else 0
    holding, spare = [largest] + [least] * (count - 1), total - largest - least * (count - 1)
    while spare > 0:
        movable = [i for i in range(1, count) if holding[i] < largest] or [i for i in range(1, count) if holding[i] < limit]
        pool, remaining = sum([weights[i] for i in movable]), spare
        for i in movable:
            more = min(limit - holding[i], max(1, remaining * weights[i] // pool), spare)
            holding[i] = holding[i] + more
            spare = spare - more
    return np.array(holding)


def centred(own_key, shape, deviation, most, cuts=(), kind=jnp.bfloat16):
    level = block_scale(own_key, shape, cuts, -0.22, 0.18) if cuts else 1.0
    entries = jax.random.normal(own_key, shape, jnp.float32) * deviation * level
    return jnp.minimum(jnp.maximum(entries, -most), most).astype(kind)


def setup_inputs(seed: int = 0) -> dict:
    key_of = jax.random.split(jax.random.key(seed), 13)
    query_proj = draw_query_proj(jax.random.fold_in(key_of[12], 71), 0)
    key_proj = draw_key_proj(jax.random.fold_in(key_of[12], 71), 0)
    value_proj = centred(key_of[2], (TOKENS, KV_HEADS * HEAD_DIM), 8.0, 48.0, ((0, 8), (1, 4)))
    query_gain = draw_query_gain(jax.random.fold_in(key_of[12], 71), 0)
    key_gain = draw_key_gain(jax.random.fold_in(key_of[12], 71), 0)
    residual = draw_residual(jax.random.fold_in(key_of[12], 71), 0)
    out_weight = centred(key_of[6], (HEADS * HEAD_DIM, D), (HEADS * HEAD_DIM) ** -0.5, 0.125, ((1, 4),))
    route_expert_keys = jax.random.split(jax.random.fold_in(key_of[7], 1), TOKENS // TOK_DEV)
    route_expert_turns = jax.random.permutation(jax.random.fold_in(key_of[7], 3), TOKENS // TOK_DEV)
    route_expert = jax.vmap(lambda own, number: assign_block(jax.random.fold_in(key_of[7], 2), own, number, TOK_DEV, EXPERTS, TOP_K, CAP, 1))(route_expert_keys, route_expert_turns).reshape((TOKENS, TOP_K))
    route_weight = jnp.clip(0.25 + 1.0 * jax.random.uniform(key_of[8], (TOKENS, TOP_K), jnp.float32) ** block_scale(key_of[8], (TOKENS, TOP_K), ((0, 8),), -0.2, 0.2), 0.25, 1.25)
    expert_gate = centred(key_of[9], (2 * EXPERTS, D, FF // 2), D ** -0.5, 0.125, ((0, 32),))
    expert_up = centred(key_of[10], (2 * EXPERTS, D, FF // 2), D ** -0.5, 0.125, ((0, 32),))
    expert_down = centred(key_of[11], (2 * EXPERTS, FF // 2, D), FF ** -0.5, 0.25, ((0, 32),))
    return dict(query_proj=query_proj, key_proj=key_proj, value_proj=value_proj, query_gain=query_gain, key_gain=key_gain, residual=residual, out_weight=out_weight, route_expert=route_expert, route_weight=route_weight, expert_gate=expert_gate, expert_up=expert_up, expert_down=expert_down)


EPSILON = 1e-06
ROPE_BASE = 10000.0

def rotation_tables(offset, count):
    pair_count = HEAD_DIM // 4
    position = offset + jnp.arange(count, dtype=jnp.int32)
    grid_row = (position // GRID_W).astype(jnp.float32)
    grid_col = (position % GRID_W).astype(jnp.float32)
    inverse = ROPE_BASE ** (-jnp.arange(pair_count, dtype=jnp.float32) / pair_count)
    angles = jnp.stack([grid_row[:, None] * inverse, grid_col[:, None] * inverse], axis=1)
    return (jnp.cos(angles), jnp.sin(angles))

def rotate(vectors, cosine_table, sine_table):
    pair_count = HEAD_DIM // 4
    shaped = vectors.reshape(vectors.shape[:-1] + (2, 2, pair_count))
    first_half = shaped[..., 0, :]
    second_half = shaped[..., 1, :]
    cosine_row = cosine_table[:, None]
    sine_row = sine_table[:, None]
    turned = jnp.stack([first_half * cosine_row - second_half * sine_row, first_half * sine_row + second_half * cosine_row], axis=-2)
    return turned.reshape(vectors.shape)

def head_norm(vectors, gain):
    scaled = vectors.astype(jnp.float32)
    scaled = scaled * lax.rsqrt(lax.optimization_barrier(jnp.mean(scaled * scaled, axis=-1, keepdims=True)) + EPSILON)
    return scaled * gain.astype(jnp.float32)

def slot_layout(choices, weights):
    token_count = choices.shape[0]
    flat_choice = choices.reshape(token_count * TOP_K).astype(jnp.int32)
    onehot = (flat_choice[:, None] == jnp.arange(EXPERTS, dtype=jnp.int32)[None, :]).astype(jnp.int32)
    earlier = jnp.cumsum(onehot, axis=0) - onehot
    slot_rank = lax.optimization_barrier(jnp.sum(earlier * onehot, axis=1))
    position = (flat_choice * CAP + slot_rank).astype(jnp.int32)
    owner = (jnp.arange(token_count * TOP_K, dtype=jnp.int32) // TOP_K).astype(jnp.int32)
    slot_token = jnp.full((EXPERTS * CAP,), token_count, jnp.int32).at[position].set(owner)
    slot_weight = jnp.zeros((EXPERTS * CAP,), jnp.float32).at[position].set(weights.reshape(token_count * TOP_K).astype(jnp.float32))
    return (slot_token, slot_weight)

def reference(query_proj, key_proj, value_proj, query_gain, key_gain, residual, out_weight, route_expert, route_weight, expert_gate, expert_up, expert_down):
    token_total = query_proj.shape[0]
    group_size = HEADS // KV_HEADS
    cosine_table, sine_table = rotation_tables(0, token_total)
    query_rot = rotate(head_norm(query_proj.reshape(token_total, HEADS, HEAD_DIM), query_gain), cosine_table, sine_table).astype(jnp.bfloat16)
    key_rot = rotate(head_norm(key_proj.reshape(token_total, KV_HEADS, HEAD_DIM), key_gain), cosine_table, sine_table).astype(jnp.bfloat16)
    value_heads = value_proj.reshape(token_total, KV_HEADS, HEAD_DIM)
    block_len = math.gcd(token_total, 1024)

    def one_head(head_index):
        query_head = lax.dynamic_index_in_dim(query_rot, head_index, 1, keepdims=False)
        key_head = lax.dynamic_index_in_dim(key_rot, head_index // group_size, 1, keepdims=False)
        value_head = lax.dynamic_index_in_dim(value_heads, head_index // group_size, 1, keepdims=False)
        query_blocks = query_head.reshape(token_total // block_len, block_len, HEAD_DIM)

        def one_block(query_block):
            scores = jnp.dot(query_block, key_head.T, preferred_element_type=jnp.float32) * HEAD_DIM ** (-0.5)
            weights = jnp.exp(scores - lax.optimization_barrier(jnp.max(scores, axis=-1, keepdims=True))).astype(jnp.bfloat16)
            weight_sum = lax.optimization_barrier(jnp.sum(weights.astype(jnp.float32), axis=-1, keepdims=True))
            summed = jnp.dot(weights, value_head, preferred_element_type=jnp.float32)
            return (summed / weight_sum).astype(jnp.bfloat16)
        return lax.map(one_block, query_blocks).reshape(token_total, HEAD_DIM)
    attended = lax.map(one_head, jnp.arange(HEADS, dtype=jnp.int32))
    attended = jnp.transpose(attended, (1, 0, 2)).reshape(token_total, HEADS * HEAD_DIM)
    mixed_sum = residual.astype(jnp.float32) + jnp.dot(attended, out_weight, preferred_element_type=jnp.float32)
    mixed_rows = mixed_sum.astype(jnp.bfloat16)
    slot_token, slot_weight = jax.vmap(slot_layout)(route_expert.reshape(N_SP, TOK_DEV, TOP_K), route_weight.reshape(N_SP, TOK_DEV, TOP_K))
    source_base = (jnp.arange(N_SP, dtype=jnp.int32) * TOK_DEV)[:, None]
    global_index = jnp.where(slot_token == TOK_DEV, token_total, slot_token + source_base).astype(jnp.int32)
    grouped_rows = mixed_rows.reshape(N_SP, TOK_DEV, D)
    padded_rows = jnp.concatenate([grouped_rows, jnp.zeros((N_SP, 1, D), jnp.bfloat16)], axis=1)

    def one_expert(routed, expert_index):
        token_ids = lax.dynamic_slice_in_dim(slot_token, expert_index * CAP, CAP, 1)
        expert_rows = jax.vmap(lambda table, index: table[index])(padded_rows, token_ids).reshape(N_SP * CAP, D)
        squares = lax.optimization_barrier(jnp.mean(jnp.square(expert_rows.astype(jnp.float32)), axis=-1, keepdims=True))
        norm_scale = lax.rsqrt(squares + EPSILON)
        total = jnp.zeros((N_SP * CAP, D), jnp.float32)
        for half in range(2):
            block = 2 * expert_index + half
            gate_value = jnp.dot(expert_rows, lax.dynamic_index_in_dim(expert_gate, block, 0, keepdims=False), preferred_element_type=jnp.float32) * norm_scale
            up_value = jnp.dot(expert_rows, lax.dynamic_index_in_dim(expert_up, block, 0, keepdims=False), preferred_element_type=jnp.float32) * norm_scale
            hidden = (jax.nn.silu(gate_value) * up_value).astype(jnp.bfloat16)
            produced = jnp.dot(hidden, lax.dynamic_index_in_dim(expert_down, block, 0, keepdims=False), preferred_element_type=jnp.float32).astype(jnp.bfloat16)
            total = total + lax.optimization_barrier(produced).astype(jnp.float32)
        slot_weights = lax.dynamic_slice_in_dim(slot_weight, expert_index * CAP, CAP, 1).reshape(N_SP * CAP)
        targets = lax.dynamic_slice_in_dim(global_index, expert_index * CAP, CAP, 1).reshape(N_SP * CAP)
        routed = routed.at[targets].add(total * slot_weights[:, None])
        return (routed, None)
    routed, unused = lax.scan(one_expert, jnp.zeros((token_total + 1, D), jnp.float32), jnp.arange(EXPERTS, dtype=jnp.int32))
    return (mixed_sum + routed[:token_total]).astype(jnp.bfloat16)
```

```python
import math

import jax
import jax.numpy as jnp
from jax import lax
from jax.sharding import PartitionSpec as P

HEAD_DIM = 64
TOP_K = 8
GRID_W = 64


EPSILON = 1e-06
ROPE_BASE = 10000.0
KEY_BLOCK = 1024


def rotation_tables(offset, count):
    pair_count = HEAD_DIM // 4
    position = offset + jnp.arange(count, dtype=jnp.int32)
    grid_row = (position // GRID_W).astype(jnp.float32)
    grid_col = (position % GRID_W).astype(jnp.float32)
    inverse = ROPE_BASE ** (-jnp.arange(pair_count, dtype=jnp.float32) / pair_count)
    angles = jnp.stack([grid_row[:, None] * inverse, grid_col[:, None] * inverse], axis=1)
    return (jnp.cos(angles), jnp.sin(angles))


def rotate(vectors, cosine_table, sine_table):
    pair_count = HEAD_DIM // 4
    shaped = vectors.reshape(vectors.shape[:-1] + (2, 2, pair_count))
    first_half = shaped[..., 0, :]
    second_half = shaped[..., 1, :]
    cosine_row = cosine_table[:, None]
    sine_row = sine_table[:, None]
    turned = jnp.stack(
        [
            first_half * cosine_row - second_half * sine_row,
            first_half * sine_row + second_half * cosine_row,
        ],
        axis=-2,
    )
    return turned.reshape(vectors.shape)


def head_norm(vectors, gain):
    scaled = vectors.astype(jnp.float32)
    scaled = scaled * lax.rsqrt(jnp.mean(scaled * scaled, axis=-1, keepdims=True) + EPSILON)
    return scaled * gain


def online_update(running, query_groups, key_block, value_block):
    running_max, running_sum, running_acc = running
    scores = jnp.einsum(
        "tkgd,nkd->kgtn", query_groups, key_block, preferred_element_type=jnp.float32
    ) * HEAD_DIM ** (-0.5)
    new_max = jnp.maximum(running_max, jnp.max(scores, axis=-1))
    rescale = jnp.exp(running_max - new_max)
    weights = jnp.exp(scores - new_max[..., None]).astype(jnp.bfloat16)
    new_sum = running_sum * rescale + jnp.sum(weights.astype(jnp.float32), axis=-1)
    update = jnp.einsum("kgtn,nkd->kgtd", weights, value_block, preferred_element_type=jnp.float32)
    return (new_max, new_sum, running_acc * rescale[..., None] + update)


def local(
    query_proj,
    key_proj,
    value_proj,
    query_gain,
    key_gain,
    residual,
    out_weight,
    route_expert,
    route_weight,
    expert_gate,
    expert_up,
    expert_down,
):
    token_count = query_proj.shape[0]
    local_heads = query_gain.shape[0]
    local_kv = key_gain.shape[0]
    group_size = local_heads // local_kv
    sp_size = lax.axis_size("sp")
    tp_size = lax.axis_size("tp")
    tp_place = lax.axis_index("tp")
    offset = lax.axis_index("sp") * token_count
    cosine_table, sine_table = rotation_tables(offset, token_count)
    query_rot = rotate(
        head_norm(query_proj.reshape(token_count, local_heads, HEAD_DIM), query_gain),
        cosine_table,
        sine_table,
    ).astype(jnp.bfloat16)
    key_rot = rotate(
        head_norm(key_proj.reshape(token_count, local_kv, HEAD_DIM), key_gain),
        cosine_table,
        sine_table,
    ).astype(jnp.bfloat16)
    packed = jnp.concatenate(
        [key_rot.reshape(token_count, local_kv * HEAD_DIM), value_proj], axis=1
    )
    query_groups = query_rot.reshape(token_count, local_kv, group_size, HEAD_DIM)
    initial = (
        jnp.full((local_kv, group_size, token_count), -1e30, jnp.float32),
        jnp.zeros((local_kv, group_size, token_count), jnp.float32),
        jnp.zeros((local_kv, group_size, token_count, HEAD_DIM), jnp.float32),
    )
    incoming = lax.all_gather(packed, "sp", axis=0, tiled=True)
    incoming_len = incoming.shape[0]
    step_len = math.gcd(incoming_len, KEY_BLOCK)

    def one_step(step_index, running):
        block_rows = lax.dynamic_slice_in_dim(incoming, step_index * step_len, step_len, 0)
        key_block = block_rows[:, : local_kv * HEAD_DIM].reshape(step_len, local_kv, HEAD_DIM)
        value_block = block_rows[:, local_kv * HEAD_DIM :].reshape(step_len, local_kv, HEAD_DIM)
        return online_update(running, query_groups, key_block, value_block)

    final_max, final_sum, final_acc = lax.fori_loop(0, incoming_len // step_len, one_step, initial)
    attended = final_acc / final_sum[..., None]
    attended = jnp.transpose(attended, (2, 0, 1, 3)).reshape(token_count, local_heads * HEAD_DIM)
    attended = attended.astype(jnp.bfloat16)
    projected = jnp.dot(
        lax.all_gather(attended, "tp", axis=1, tiled=True),
        out_weight,
        preferred_element_type=jnp.float32,
    )
    mixed_sum = residual.astype(jnp.float32) + projected
    mixed_rows = mixed_sum.astype(jnp.bfloat16)
    full_rows = lax.all_gather(mixed_rows, "tp", axis=1, tiled=True)
    width_total = full_rows.shape[1]
    per_sp = tp_size // 2
    column = tp_place // 2
    experts_total = per_sp * sp_size
    capacity = 3 * token_count * TOP_K // (2 * experts_total)
    slot_count = sp_size * capacity
    flat_choice = route_expert.reshape(token_count * TOP_K)
    onehot = (flat_choice[:, None] == jnp.arange(experts_total, dtype=jnp.int32)[None, :]).astype(
        jnp.int32
    )
    earlier = jnp.cumsum(onehot, axis=0) - onehot
    slot_rank = jnp.sum(earlier * onehot, axis=1)
    mine = flat_choice % per_sp == column
    target = flat_choice // per_sp * capacity + slot_rank
    owner = jnp.arange(token_count * TOP_K, dtype=jnp.int32) // TOP_K
    slot_token = (
        jnp.full((slot_count + 1,), token_count, jnp.int32)
        .at[jnp.where(mine, target, slot_count)]
        .set(owner)[:slot_count]
    )
    padded = jnp.concatenate([full_rows, jnp.zeros((1, width_total), jnp.bfloat16)], axis=0)
    selected = padded[slot_token].reshape(sp_size, capacity, width_total)
    arrived = lax.all_to_all(selected, "sp", split_axis=0, concat_axis=0, tiled=True)
    expert_rows = arrived.reshape(slot_count, width_total)
    squares = jnp.mean(jnp.square(expert_rows.astype(jnp.float32)), axis=-1, keepdims=True)
    norm_scale = lax.rsqrt(squares + EPSILON)
    gate_value = (
        jnp.dot(expert_rows, expert_gate[0], preferred_element_type=jnp.float32) * norm_scale
    )
    up_value = jnp.dot(expert_rows, expert_up[0], preferred_element_type=jnp.float32) * norm_scale
    hidden = (jax.nn.silu(gate_value) * up_value).astype(jnp.bfloat16)
    half_result = jnp.dot(hidden, expert_down[0], preferred_element_type=jnp.float32).astype(
        jnp.bfloat16
    )
    returned = lax.all_to_all(
        half_result.reshape(sp_size, capacity, width_total),
        "sp",
        split_axis=0,
        concat_axis=0,
        tiled=True,
    )
    slot_results = returned.reshape(slot_count, width_total)
    mine_grid = mine.reshape(token_count, TOP_K)
    target_grid = target.reshape(token_count, TOP_K)
    gathered_sum = jnp.zeros((token_count, width_total), jnp.float32)
    for choice_index in range(TOP_K):
        chosen = mine_grid[:, choice_index]
        index = jnp.where(chosen, target_grid[:, choice_index], 0)
        factor = jnp.where(chosen, route_weight[:, choice_index], 0.0)
        picked = slot_results[index].astype(jnp.float32)
        gathered_sum = gathered_sum + factor[:, None] * picked
    routed = lax.psum_scatter(
        gathered_sum.astype(jnp.bfloat16), "tp", scatter_dimension=1, tiled=True
    ).astype(jnp.float32)
    return (mixed_sum + routed).astype(jnp.bfloat16)


def normed_heads(proj, gain, cosine_table, sine_table):
    token_count = proj.shape[0]
    heads = proj.reshape(token_count, gain.shape[0], HEAD_DIM)
    return rotate(head_norm(heads, gain), cosine_table, sine_table).astype(jnp.bfloat16)


def flip(value, axis, mask):
    return lax.ppermute(value, axis, [(i, i ^ mask) for i in range(lax.axis_size(axis))])


def grid_gather(block):
    half = block.shape[0] // 2
    from_x = flip(block, "tp", 1)
    from_y = flip(block, "tp", 2)
    upper = flip(from_y[:half], "tp", 1)
    lower = flip(from_x[half:], "tp", 2)
    return [block, from_x, from_y, jnp.concatenate([upper, lower], axis=0)]


def add_rounded(mine, other):
    return (mine.astype(jnp.float32) + other.astype(jnp.float32)).astype(jnp.bfloat16)


def grid_scatter_sum(blocks):
    rows, width = blocks.shape[0] // 2, blocks.shape[1] // 4
    upper = [blocks[:rows, q * width : (q + 1) * width] for q in range(4)]
    lower = [blocks[rows:, q * width : (q + 1) * width] for q in range(4)]
    got_x = flip(jnp.concatenate([upper[1], upper[3]], axis=0), "tp", 1)
    got_y = flip(jnp.concatenate([lower[2], lower[3]], axis=0), "tp", 2)
    pass_y = flip(add_rounded(upper[2], got_x[rows:]), "tp", 2)
    pass_x = flip(add_rounded(lower[1], got_y[rows:]), "tp", 1)
    f32 = jnp.float32
    top = upper[0].astype(f32) + got_x[:rows].astype(f32) + pass_y.astype(f32)
    bottom = lower[0].astype(f32) + got_y[:rows].astype(f32) + pass_x.astype(f32)
    return jnp.concatenate([top, bottom], axis=0)


def relative_blocks(weight, place, axis):
    width = weight.shape[axis] // 4
    return jnp.concatenate(
        [lax.dynamic_slice_in_dim(weight, (place ^ q) * width, width, axis) for q in range(4)],
        axis=axis,
    )


def local_dense(
    query_proj,
    key_proj,
    value_proj,
    query_gain,
    key_gain,
    residual,
    out_weight,
    route_expert,
    route_weight,
    expert_gate,
    expert_up,
    expert_down,
):
    token_count = query_proj.shape[0]
    local_heads = query_gain.shape[0]
    local_kv = key_gain.shape[0]
    group_size = local_heads // local_kv
    sp_size = lax.axis_size("sp")
    tp_size = lax.axis_size("tp")
    sp_place = lax.axis_index("sp")
    tp_place = lax.axis_index("tp")
    chips = sp_size // 2
    experts_total = sp_size * tp_size // 2
    my_expert = (sp_place * tp_size + tp_place) // 2
    cosine_table, sine_table = rotation_tables(sp_place * token_count, token_count)

    key_rot = normed_heads(key_proj, key_gain, cosine_table, sine_table)
    packed = jnp.concatenate(
        [key_rot.reshape(token_count, local_kv * HEAD_DIM), value_proj], axis=1
    )
    kv_blocks = [packed] + [flip(packed, "sp", 2 * d) for d in range(1, chips)]

    ids = jnp.arange(experts_total, dtype=jnp.int32)
    chosen = route_expert.T[None, :, :] == ids[:, None, None]
    table = jnp.sum(jnp.where(chosen, route_weight.T[None, :, :], 0.0), axis=1)
    tables = jnp.stack([table] + [flip(table, "sp", 2 * d) for d in range(1, chips)])
    tables = jnp.stack([tables, flip(tables, "sp", 1)])
    factors = jnp.sum(jnp.where(ids[:, None] == my_expert, tables, 0.0), axis=2)

    query_rot = normed_heads(query_proj, query_gain, cosine_table, sine_table)
    query_groups = query_rot.reshape(token_count, local_kv, group_size, HEAD_DIM)
    running = (
        jnp.full((local_kv, group_size, token_count), -1e30, jnp.float32),
        jnp.zeros((local_kv, group_size, token_count), jnp.float32),
        jnp.zeros((local_kv, group_size, token_count, HEAD_DIM), jnp.float32),
    )
    for block in kv_blocks:
        both = jnp.concatenate([block, flip(block, "sp", 1)], axis=0)
        key_block = both[:, : local_kv * HEAD_DIM].reshape(-1, local_kv, HEAD_DIM)
        value_block = both[:, local_kv * HEAD_DIM :].reshape(-1, local_kv, HEAD_DIM)
        running = online_update(running, query_groups, key_block, value_block)
    final_max, final_sum, final_acc = running
    attended = final_acc / final_sum[..., None]
    attended = jnp.transpose(attended, (2, 0, 1, 3)).reshape(token_count, local_heads * HEAD_DIM)
    attended = attended.astype(jnp.bfloat16)

    out_relative = relative_blocks(out_weight, tp_place, 0)
    gate_up = relative_blocks(
        jnp.concatenate([expert_gate[0], expert_up[0]], axis=1), tp_place, 0
    )
    down = relative_blocks(expert_down[0], tp_place, 1)
    hidden_units = expert_down.shape[1]

    projected = jnp.dot(
        jnp.concatenate(grid_gather(attended), axis=1),
        out_relative,
        preferred_element_type=jnp.float32,
    )
    mixed_sum = residual.astype(jnp.float32) + projected
    mixed_rows = mixed_sum.astype(jnp.bfloat16)

    def half_expert(rows, factor):
        squares = jnp.mean(jnp.square(rows.astype(jnp.float32)), axis=-1, keepdims=True)
        norm_scale = lax.rsqrt(squares + EPSILON)
        both = jnp.dot(rows, gate_up, preferred_element_type=jnp.float32) * norm_scale
        gate_value, up_value = both[:, :hidden_units], both[:, hidden_units:]
        hidden = (jax.nn.silu(gate_value) * up_value).astype(jnp.bfloat16)
        half_result = jnp.dot(hidden, down, preferred_element_type=jnp.float32)
        half_result = half_result.astype(jnp.bfloat16).astype(jnp.float32)
        return (half_result * factor[:, None]).astype(jnp.bfloat16)

    blocks = [mixed_rows] + [flip(mixed_rows, "sp", 2 * d) for d in range(1, chips)]
    result = mixed_sum
    for d, block in enumerate(blocks):
        rows = jnp.concatenate(grid_gather(block), axis=1)
        other_rows = flip(rows, "sp", 1)
        theirs = flip(half_expert(other_rows, factors[1, d]), "sp", 1)
        mine = add_rounded(half_expert(rows, factors[0, d]), theirs)
        summed = grid_scatter_sum(mine)
        if d:
            summed = flip(summed.astype(jnp.bfloat16), "sp", 2 * d).astype(jnp.float32)
        result = result + summed
    return result.astype(jnp.bfloat16)


def takes_dense(mesh):
    chips = mesh.shape["sp"] // 2
    experts_total = mesh.shape["sp"] * mesh.shape["tp"] // 2
    power = mesh.shape["sp"] % 2 == 0 and chips & (chips - 1) == 0
    return mesh.shape["tp"] == 4 and power and experts_total <= 2 * TOP_K


def solution(mesh):
    in_specs = (
        P("sp", "tp"),
        P("sp", "tp"),
        P("sp", "tp"),
        P("tp", None),
        P("tp", None),
        P("sp", "tp"),
        P(None, "tp"),
        P("sp", None),
        P("sp", None),
        P(("sp", "tp"), None, None),
        P(("sp", "tp"), None, None),
        P(("sp", "tp"), None, None),
    )
    out_specs = P("sp", "tp")
    body = local_dense if takes_dense(mesh) else local
    return jax.shard_map(body, mesh=mesh, in_specs=in_specs, out_specs=out_specs, check_vma=False)
```

```python
import functools
import math

import jax
import jax.numpy as jnp
from jax import lax
from jax.experimental import pallas as pl
from jax.experimental.pallas import tpu as pltpu
from jax.sharding import PartitionSpec as P

HEAD_DIM = 64
TOP_K = 8
GRID_W = 64


EPSILON = 1e-06
ROPE_BASE = 10000.0
KEY_BLOCK = 1024


def rotation_tables(offset, count):
    pair_count = HEAD_DIM // 4
    position = offset + jnp.arange(count, dtype=jnp.int32)
    grid_row = (position // GRID_W).astype(jnp.float32)
    grid_col = (position % GRID_W).astype(jnp.float32)
    inverse = ROPE_BASE ** (-jnp.arange(pair_count, dtype=jnp.float32) / pair_count)
    angles = jnp.stack([grid_row[:, None] * inverse, grid_col[:, None] * inverse], axis=1)
    return (jnp.cos(angles), jnp.sin(angles))


def rotate(vectors, cosine_table, sine_table):
    pair_count = HEAD_DIM // 4
    shaped = vectors.reshape(vectors.shape[:-1] + (2, 2, pair_count))
    first_half = shaped[..., 0, :]
    second_half = shaped[..., 1, :]
    cosine_row = cosine_table[:, None]
    sine_row = sine_table[:, None]
    turned = jnp.stack(
        [
            first_half * cosine_row - second_half * sine_row,
            first_half * sine_row + second_half * cosine_row,
        ],
        axis=-2,
    )
    return turned.reshape(vectors.shape)


def head_norm(vectors, gain):
    scaled = vectors.astype(jnp.float32)
    scaled = scaled * lax.rsqrt(jnp.mean(scaled * scaled, axis=-1, keepdims=True) + EPSILON)
    return scaled * gain


def online_update(running, query_groups, key_block, value_block):
    running_max, running_sum, running_acc = running
    scores = jnp.einsum(
        "tkgd,nkd->kgtn", query_groups, key_block, preferred_element_type=jnp.float32
    ) * HEAD_DIM ** (-0.5)
    new_max = jnp.maximum(running_max, jnp.max(scores, axis=-1))
    rescale = jnp.exp(running_max - new_max)
    weights = jnp.exp(scores - new_max[..., None]).astype(jnp.bfloat16)
    new_sum = running_sum * rescale + jnp.sum(weights.astype(jnp.float32), axis=-1)
    update = jnp.einsum("kgtn,nkd->kgtd", weights, value_block, preferred_element_type=jnp.float32)
    return (new_max, new_sum, running_acc * rescale[..., None] + update)


def local(
    query_proj,
    key_proj,
    value_proj,
    query_gain,
    key_gain,
    residual,
    out_weight,
    route_expert,
    route_weight,
    expert_gate,
    expert_up,
    expert_down,
):
    token_count = query_proj.shape[0]
    local_heads = query_gain.shape[0]
    local_kv = key_gain.shape[0]
    group_size = local_heads // local_kv
    sp_size = lax.axis_size("sp")
    tp_size = lax.axis_size("tp")
    tp_place = lax.axis_index("tp")
    offset = lax.axis_index("sp") * token_count
    cosine_table, sine_table = rotation_tables(offset, token_count)
    query_rot = rotate(
        head_norm(query_proj.reshape(token_count, local_heads, HEAD_DIM), query_gain),
        cosine_table,
        sine_table,
    ).astype(jnp.bfloat16)
    key_rot = rotate(
        head_norm(key_proj.reshape(token_count, local_kv, HEAD_DIM), key_gain),
        cosine_table,
        sine_table,
    ).astype(jnp.bfloat16)
    packed = jnp.concatenate(
        [key_rot.reshape(token_count, local_kv * HEAD_DIM), value_proj], axis=1
    )
    query_groups = query_rot.reshape(token_count, local_kv, group_size, HEAD_DIM)
    initial = (
        jnp.full((local_kv, group_size, token_count), -1e30, jnp.float32),
        jnp.zeros((local_kv, group_size, token_count), jnp.float32),
        jnp.zeros((local_kv, group_size, token_count, HEAD_DIM), jnp.float32),
    )
    incoming = lax.all_gather(packed, "sp", axis=0, tiled=True)
    incoming_len = incoming.shape[0]
    step_len = math.gcd(incoming_len, KEY_BLOCK)

    def one_step(step_index, running):
        block_rows = lax.dynamic_slice_in_dim(incoming, step_index * step_len, step_len, 0)
        key_block = block_rows[:, : local_kv * HEAD_DIM].reshape(step_len, local_kv, HEAD_DIM)
        value_block = block_rows[:, local_kv * HEAD_DIM :].reshape(step_len, local_kv, HEAD_DIM)
        return online_update(running, query_groups, key_block, value_block)

    final_max, final_sum, final_acc = lax.fori_loop(0, incoming_len // step_len, one_step, initial)
    attended = final_acc / final_sum[..., None]
    attended = jnp.transpose(attended, (2, 0, 1, 3)).reshape(token_count, local_heads * HEAD_DIM)
    attended = attended.astype(jnp.bfloat16)
    projected = jnp.dot(
        lax.all_gather(attended, "tp", axis=1, tiled=True),
        out_weight,
        preferred_element_type=jnp.float32,
    )
    mixed_sum = residual.astype(jnp.float32) + projected
    mixed_rows = mixed_sum.astype(jnp.bfloat16)
    full_rows = lax.all_gather(mixed_rows, "tp", axis=1, tiled=True)
    width_total = full_rows.shape[1]
    per_sp = tp_size // 2
    column = tp_place // 2
    experts_total = per_sp * sp_size
    capacity = 3 * token_count * TOP_K // (2 * experts_total)
    slot_count = sp_size * capacity
    flat_choice = route_expert.reshape(token_count * TOP_K)
    onehot = (flat_choice[:, None] == jnp.arange(experts_total, dtype=jnp.int32)[None, :]).astype(
        jnp.int32
    )
    earlier = jnp.cumsum(onehot, axis=0) - onehot
    slot_rank = jnp.sum(earlier * onehot, axis=1)
    mine = flat_choice % per_sp == column
    target = flat_choice // per_sp * capacity + slot_rank
    owner = jnp.arange(token_count * TOP_K, dtype=jnp.int32) // TOP_K
    slot_token = (
        jnp.full((slot_count + 1,), token_count, jnp.int32)
        .at[jnp.where(mine, target, slot_count)]
        .set(owner)[:slot_count]
    )
    padded = jnp.concatenate([full_rows, jnp.zeros((1, width_total), jnp.bfloat16)], axis=0)
    selected = padded[slot_token].reshape(sp_size, capacity, width_total)
    arrived = lax.all_to_all(selected, "sp", split_axis=0, concat_axis=0, tiled=True)
    expert_rows = arrived.reshape(slot_count, width_total)
    squares = jnp.mean(jnp.square(expert_rows.astype(jnp.float32)), axis=-1, keepdims=True)
    norm_scale = lax.rsqrt(squares + EPSILON)
    gate_value = (
        jnp.dot(expert_rows, expert_gate[0], preferred_element_type=jnp.float32) * norm_scale
    )
    up_value = jnp.dot(expert_rows, expert_up[0], preferred_element_type=jnp.float32) * norm_scale
    hidden = (jax.nn.silu(gate_value) * up_value).astype(jnp.bfloat16)
    half_result = jnp.dot(hidden, expert_down[0], preferred_element_type=jnp.float32).astype(
        jnp.bfloat16
    )
    returned = lax.all_to_all(
        half_result.reshape(sp_size, capacity, width_total),
        "sp",
        split_axis=0,
        concat_axis=0,
        tiled=True,
    )
    slot_results = returned.reshape(slot_count, width_total)
    mine_grid = mine.reshape(token_count, TOP_K)
    target_grid = target.reshape(token_count, TOP_K)
    gathered_sum = jnp.zeros((token_count, width_total), jnp.float32)
    for choice_index in range(TOP_K):
        chosen = mine_grid[:, choice_index]
        index = jnp.where(chosen, target_grid[:, choice_index], 0)
        factor = jnp.where(chosen, route_weight[:, choice_index], 0.0)
        picked = slot_results[index].astype(jnp.float32)
        gathered_sum = gathered_sum + factor[:, None] * picked
    routed = lax.psum_scatter(
        gathered_sum.astype(jnp.bfloat16), "tp", scatter_dimension=1, tiled=True
    ).astype(jnp.float32)
    return (mixed_sum + routed).astype(jnp.bfloat16)


def normed_heads(proj, gain, cosine_table, sine_table):
    token_count = proj.shape[0]
    heads = proj.reshape(token_count, gain.shape[0], HEAD_DIM)
    return rotate(head_norm(heads, gain), cosine_table, sine_table).astype(jnp.bfloat16)


def flip(value, axis, mask):
    return lax.ppermute(value, axis, [(i, i ^ mask) for i in range(lax.axis_size(axis))])


def grid_gather(block):
    half = block.shape[0] // 2
    from_x = flip(block, "tp", 1)
    from_y = flip(block, "tp", 2)
    upper = flip(from_y[:half], "tp", 1)
    lower = flip(from_x[half:], "tp", 2)
    return [block, from_x, from_y, jnp.concatenate([upper, lower], axis=0)]


def add_rounded(mine, other):
    return (mine.astype(jnp.float32) + other.astype(jnp.float32)).astype(jnp.bfloat16)


def relative_blocks(weight, place, axis):
    width = weight.shape[axis] // 4
    return jnp.concatenate(
        [lax.dynamic_slice_in_dim(weight, (place ^ q) * width, width, axis) for q in range(4)],
        axis=axis,
    )


def flip_index(index, mask):
    bit = 1
    while bit <= mask:
        if mask & bit:
            index = index + bit - 2 * bit * ((index // bit) % 2)
        bit *= 2
    return index


KINDS = 12
Z_OUT, X_ONE, Y_ONE, X_TWO, Y_TWO, CORE_OUT, CORE_BACK, X_SUM, Y_SUM, Y_PASS, X_PASS, Z_BACK = range(
    KINDS
)


def experts_kernel(
    chips,
    x_ref,
    gate_up_ref,
    down_ref,
    factor_ref,
    out_ref,
    rows,
    outs,
    core_in,
    send_x,
    send_y,
    got_x,
    got_y,
    pass_y,
    pass_x,
    end_y,
    end_x,
    send_z,
    got_z,
    send_sem,
    recv_sem,
):
    sp_place, tp_place = lax.axis_index("sp"), lax.axis_index("tp")
    over_x = {"tp": flip_index(tp_place, 1)}
    over_y = {"tp": flip_index(tp_place, 2)}
    core = {"sp": flip_index(sp_place, 1)}
    over_z = [{"sp": flip_index(sp_place, 2 * d)} for d in range(1, chips)]
    f32, bf16 = jnp.float32, jnp.bfloat16
    count, width = x_ref.shape
    half = count // 2
    hidden_units = down_ref.shape[0]
    upper, lower = pl.ds(0, half), pl.ds(half, half)

    def quarter(q):
        return pl.ds(q * width, width)

    barrier = pltpu.get_barrier_semaphore()
    partners = [over_x, over_y, core] + over_z
    for partner in partners:
        pl.semaphore_signal(
            barrier, inc=1, device_id=partner, device_id_type=pl.DeviceIdType.MESH
        )
    pl.semaphore_wait(barrier, len(partners))

    copies = {}

    def send(kind, d, src, dst, device):
        copies[kind, d] = pltpu.make_async_remote_copy(
            src_ref=src,
            dst_ref=dst,
            send_sem=send_sem.at[kind, d],
            recv_sem=recv_sem.at[kind, d],
            device_id=device,
            device_id_type=pl.DeviceIdType.MESH,
        )
        copies[kind, d].start()

    def arrived(kind, d):
        copies[kind, d].wait_recv()

    def spread(d):
        if d:
            arrived(Z_OUT, d)
            block = rows.at[d, 0, :, quarter(0)]
        else:
            block = x_ref
        send(X_ONE, d, block, rows.at[d, 0, :, quarter(1)], over_x)
        send(Y_ONE, d, block, rows.at[d, 0, :, quarter(2)], over_y)

    def spread_on(d):
        arrived(Y_ONE, d)
        send(X_TWO, d, rows.at[d, 0, upper, quarter(2)], rows.at[d, 0, upper, quarter(3)], over_x)
        arrived(X_ONE, d)
        send(Y_TWO, d, rows.at[d, 0, lower, quarter(1)], rows.at[d, 0, lower, quarter(3)], over_y)

    def swap_cores(d):
        arrived(X_TWO, d)
        arrived(Y_TWO, d)
        send(CORE_OUT, d, rows.at[d, 0], rows.at[d, 1], core)

    def compute(d):
        arrived(CORE_OUT, d)

        def one(i, carry):
            side = 1 - i
            own_rows = rows[d, side]
            wide = own_rows.astype(f32)
            squares = jnp.mean(wide * wide, axis=-1, keepdims=True)
            norm_scale = lax.rsqrt(squares + EPSILON)
            both = jnp.dot(own_rows, gate_up_ref[...], preferred_element_type=f32) * norm_scale
            gate_value, up_value = both[:, :hidden_units], both[:, hidden_units:]
            hidden = (gate_value / (1.0 + jnp.exp(-gate_value)) * up_value).astype(bf16)
            factor = factor_ref[d, side]
            for q in range(4):
                part = jnp.dot(hidden, down_ref[:, quarter(q)], preferred_element_type=f32)
                outs[d, side, :, quarter(q)] = (part.astype(bf16).astype(f32) * factor).astype(bf16)
            return carry

        lax.fori_loop(0, 2, one, 0)
        send(CORE_BACK, d, outs.at[d, 1], core_in.at[d], core)

    def both_cores(d, span, q):
        mine = outs[d, 0, span, quarter(q)].astype(f32)
        return (mine + core_in[d, span, quarter(q)].astype(f32)).astype(bf16)

    def gather_sums(d):
        arrived(CORE_BACK, d)
        send_x[d, :, quarter(0)] = both_cores(d, upper, 1)
        send_x[d, :, quarter(1)] = both_cores(d, upper, 3)
        send(X_SUM, d, send_x.at[d], got_x.at[d], over_x)
        send_y[d, :, quarter(0)] = both_cores(d, lower, 2)
        send_y[d, :, quarter(1)] = both_cores(d, lower, 3)
        send(Y_SUM, d, send_y.at[d], got_y.at[d], over_y)

    def pass_sums(d):
        arrived(X_SUM, d)
        pass_y[d] = add_rounded(both_cores(d, upper, 2), got_x[d, :, quarter(1)])
        send(Y_PASS, d, pass_y.at[d], end_y.at[d], over_y)
        arrived(Y_SUM, d)
        pass_x[d] = add_rounded(both_cores(d, lower, 1), got_y[d, :, quarter(1)])
        send(X_PASS, d, pass_x.at[d], end_x.at[d], over_x)

    def finish(d):
        arrived(Y_PASS, d)
        top = both_cores(d, upper, 0).astype(f32) + got_x[d, :, quarter(0)].astype(f32)
        top = top + end_y[d].astype(f32)
        arrived(X_PASS, d)
        bottom = both_cores(d, lower, 0).astype(f32) + got_y[d, :, quarter(0)].astype(f32)
        bottom = bottom + end_x[d].astype(f32)
        if d:
            send_z[d, upper, :] = top.astype(bf16)
            send_z[d, lower, :] = bottom.astype(bf16)
            send(Z_BACK, d, send_z.at[d], got_z.at[d], over_z[d - 1])
        else:
            out_ref[upper, :] = top
            out_ref[lower, :] = bottom

    for d in range(1, chips):
        send(Z_OUT, d, x_ref, rows.at[d, 0, :, quarter(0)], over_z[d - 1])
    rows[0, 0, :, quarter(0)] = x_ref[...]
    stages = (
        (0, spread),
        (1, spread_on),
        (2, swap_cores),
        (3, gather_sums),
        (4, pass_sums),
        (5, finish),
        (2, compute),
    )
    for step in range(chips + 5):
        for delay, stage in stages:
            if 0 <= step - delay < chips:
                stage(step - delay)
    for d in range(1, chips):
        arrived(Z_BACK, d)
        out_ref[...] += got_z[d].astype(f32)
    for copy in copies.values():
        copy.wait_send()


def routed_experts(mixed_rows, gate_up, down, factors):
    chips = factors.shape[0]
    count, width = mixed_rows.shape
    half, total = count // 2, down.shape[1]
    bf16 = jnp.bfloat16
    shapes = [
        (chips, 2, count, total),
        (chips, 2, count, total),
        (chips, count, total),
        (chips, half, 2 * width),
        (chips, half, 2 * width),
        (chips, half, 2 * width),
        (chips, half, 2 * width),
        (chips, half, width),
        (chips, half, width),
        (chips, half, width),
        (chips, half, width),
        (chips, count, width),
        (chips, count, width),
    ]
    sems = pltpu.SemaphoreType.DMA((KINDS, chips))
    return pl.pallas_call(
        functools.partial(experts_kernel, chips),
        out_shape=jax.ShapeDtypeStruct((count, width), jnp.float32),
        in_specs=[pl.BlockSpec(memory_space=pltpu.VMEM)] * 4,
        out_specs=pl.BlockSpec(memory_space=pltpu.VMEM),
        scratch_shapes=[pltpu.VMEM(shape, bf16) for shape in shapes] + [sems, sems],
        compiler_params=pltpu.CompilerParams(
            collective_id=0, has_side_effects=True, vmem_limit_bytes=52 * 1024 * 1024
        ),
    )(mixed_rows, gate_up, down, factors)


def local_dense(
    query_proj,
    key_proj,
    value_proj,
    query_gain,
    key_gain,
    residual,
    out_weight,
    route_expert,
    route_weight,
    expert_gate,
    expert_up,
    expert_down,
):
    token_count = query_proj.shape[0]
    local_heads = query_gain.shape[0]
    local_kv = key_gain.shape[0]
    group_size = local_heads // local_kv
    sp_size = lax.axis_size("sp")
    tp_size = lax.axis_size("tp")
    sp_place = lax.axis_index("sp")
    tp_place = lax.axis_index("tp")
    chips = sp_size // 2
    experts_total = sp_size * tp_size // 2
    my_expert = (sp_place * tp_size + tp_place) // 2
    cosine_table, sine_table = rotation_tables(sp_place * token_count, token_count)

    key_rot = normed_heads(key_proj, key_gain, cosine_table, sine_table)
    packed = jnp.concatenate(
        [key_rot.reshape(token_count, local_kv * HEAD_DIM), value_proj], axis=1
    )
    kv_blocks = [packed] + [flip(packed, "sp", 2 * d) for d in range(1, chips)]

    ids = jnp.arange(experts_total, dtype=jnp.int32)
    chosen = route_expert.T[None, :, :] == ids[:, None, None]
    table = jnp.sum(jnp.where(chosen, route_weight.T[None, :, :], 0.0), axis=1)
    tables = jnp.stack([table] + [flip(table, "sp", 2 * d) for d in range(1, chips)])
    tables = jnp.stack([tables, flip(tables, "sp", 1)])
    factors = jnp.sum(jnp.where(ids[:, None] == my_expert, tables, 0.0), axis=2)

    query_rot = normed_heads(query_proj, query_gain, cosine_table, sine_table)
    query_groups = query_rot.reshape(token_count, local_kv, group_size, HEAD_DIM)
    running = (
        jnp.full((local_kv, group_size, token_count), -1e30, jnp.float32),
        jnp.zeros((local_kv, group_size, token_count), jnp.float32),
        jnp.zeros((local_kv, group_size, token_count, HEAD_DIM), jnp.float32),
    )
    for block in kv_blocks:
        both = jnp.concatenate([block, flip(block, "sp", 1)], axis=0)
        key_block = both[:, : local_kv * HEAD_DIM].reshape(-1, local_kv, HEAD_DIM)
        value_block = both[:, local_kv * HEAD_DIM :].reshape(-1, local_kv, HEAD_DIM)
        running = online_update(running, query_groups, key_block, value_block)
    final_max, final_sum, final_acc = running
    attended = final_acc / final_sum[..., None]
    attended = jnp.transpose(attended, (2, 0, 1, 3)).reshape(token_count, local_heads * HEAD_DIM)
    attended = attended.astype(jnp.bfloat16)

    out_relative = relative_blocks(out_weight, tp_place, 0)
    gate_up = relative_blocks(
        jnp.concatenate([expert_gate[0], expert_up[0]], axis=1), tp_place, 0
    )
    down = relative_blocks(expert_down[0], tp_place, 1)
    hidden_units = expert_down.shape[1]

    projected = jnp.dot(
        jnp.concatenate(grid_gather(attended), axis=1),
        out_relative,
        preferred_element_type=jnp.float32,
    )
    mixed_sum = residual.astype(jnp.float32) + projected
    mixed_rows = mixed_sum.astype(jnp.bfloat16)

    columns = jnp.transpose(factors, (1, 0, 2))[..., None]
    result = mixed_sum + routed_experts(mixed_rows, gate_up, down, columns)
    return result.astype(jnp.bfloat16)


def takes_dense(mesh):
    chips = mesh.shape["sp"] // 2
    experts_total = mesh.shape["sp"] * mesh.shape["tp"] // 2
    power = mesh.shape["sp"] % 2 == 0 and chips & (chips - 1) == 0
    return mesh.shape["tp"] == 4 and power and experts_total <= 2 * TOP_K


def solution(mesh):
    in_specs = (
        P("sp", "tp"),
        P("sp", "tp"),
        P("sp", "tp"),
        P("tp", None),
        P("tp", None),
        P("sp", "tp"),
        P(None, "tp"),
        P("sp", None),
        P("sp", None),
        P(("sp", "tp"), None, None),
        P(("sp", "tp"), None, None),
        P(("sp", "tp"), None, None),
    )
    out_specs = P("sp", "tp")
    body = local_dense if takes_dense(mesh) else local
    return jax.shard_map(body, mesh=mesh, in_specs=in_specs, out_specs=out_specs, check_vma=False)
```

```python
import functools
import math

import jax
import jax.numpy as jnp
from jax import lax
from jax.experimental import pallas as pl
from jax.experimental.pallas import tpu as pltpu
from jax.sharding import PartitionSpec as P

HEAD_DIM = 64
TOP_K = 8
GRID_W = 64


EPSILON = 1e-06
ROPE_BASE = 10000.0
KEY_BLOCK = 1024


def rotation_tables(offset, count):
    pair_count = HEAD_DIM // 4
    position = offset + jnp.arange(count, dtype=jnp.int32)
    grid_row = (position // GRID_W).astype(jnp.float32)
    grid_col = (position % GRID_W).astype(jnp.float32)
    inverse = ROPE_BASE ** (-jnp.arange(pair_count, dtype=jnp.float32) / pair_count)
    angles = jnp.stack([grid_row[:, None] * inverse, grid_col[:, None] * inverse], axis=1)
    return (jnp.cos(angles), jnp.sin(angles))


def rotate(vectors, cosine_table, sine_table):
    pair_count = HEAD_DIM // 4
    shaped = vectors.reshape(vectors.shape[:-1] + (2, 2, pair_count))
    first_half = shaped[..., 0, :]
    second_half = shaped[..., 1, :]
    cosine_row = cosine_table[:, None]
    sine_row = sine_table[:, None]
    turned = jnp.stack(
        [
            first_half * cosine_row - second_half * sine_row,
            first_half * sine_row + second_half * cosine_row,
        ],
        axis=-2,
    )
    return turned.reshape(vectors.shape)


def head_norm(vectors, gain):
    scaled = vectors.astype(jnp.float32)
    scaled = scaled * lax.rsqrt(jnp.mean(scaled * scaled, axis=-1, keepdims=True) + EPSILON)
    return scaled * gain


def online_update(running, query_groups, key_block, value_block):
    running_max, running_sum, running_acc = running
    scores = jnp.einsum(
        "tkgd,nkd->kgtn", query_groups, key_block, preferred_element_type=jnp.float32
    ) * HEAD_DIM ** (-0.5)
    new_max = jnp.maximum(running_max, jnp.max(scores, axis=-1))
    rescale = jnp.exp(running_max - new_max)
    weights = jnp.exp(scores - new_max[..., None]).astype(jnp.bfloat16)
    new_sum = running_sum * rescale + jnp.sum(weights.astype(jnp.float32), axis=-1)
    update = jnp.einsum("kgtn,nkd->kgtd", weights, value_block, preferred_element_type=jnp.float32)
    return (new_max, new_sum, running_acc * rescale[..., None] + update)


def local(
    query_proj,
    key_proj,
    value_proj,
    query_gain,
    key_gain,
    residual,
    out_weight,
    route_expert,
    route_weight,
    expert_gate,
    expert_up,
    expert_down,
):
    token_count = query_proj.shape[0]
    local_heads = query_gain.shape[0]
    local_kv = key_gain.shape[0]
    group_size = local_heads // local_kv
    sp_size = lax.axis_size("sp")
    tp_size = lax.axis_size("tp")
    tp_place = lax.axis_index("tp")
    offset = lax.axis_index("sp") * token_count
    cosine_table, sine_table = rotation_tables(offset, token_count)
    query_rot = rotate(
        head_norm(query_proj.reshape(token_count, local_heads, HEAD_DIM), query_gain),
        cosine_table,
        sine_table,
    ).astype(jnp.bfloat16)
    key_rot = rotate(
        head_norm(key_proj.reshape(token_count, local_kv, HEAD_DIM), key_gain),
        cosine_table,
        sine_table,
    ).astype(jnp.bfloat16)
    packed = jnp.concatenate(
        [key_rot.reshape(token_count, local_kv * HEAD_DIM), value_proj], axis=1
    )
    query_groups = query_rot.reshape(token_count, local_kv, group_size, HEAD_DIM)
    initial = (
        jnp.full((local_kv, group_size, token_count), -1e30, jnp.float32),
        jnp.zeros((local_kv, group_size, token_count), jnp.float32),
        jnp.zeros((local_kv, group_size, token_count, HEAD_DIM), jnp.float32),
    )
    incoming = lax.all_gather(packed, "sp", axis=0, tiled=True)
    incoming_len = incoming.shape[0]
    step_len = math.gcd(incoming_len, KEY_BLOCK)

    def one_step(step_index, running):
        block_rows = lax.dynamic_slice_in_dim(incoming, step_index * step_len, step_len, 0)
        key_block = block_rows[:, : local_kv * HEAD_DIM].reshape(step_len, local_kv, HEAD_DIM)
        value_block = block_rows[:, local_kv * HEAD_DIM :].reshape(step_len, local_kv, HEAD_DIM)
        return online_update(running, query_groups, key_block, value_block)

    final_max, final_sum, final_acc = lax.fori_loop(0, incoming_len // step_len, one_step, initial)
    attended = final_acc / final_sum[..., None]
    attended = jnp.transpose(attended, (2, 0, 1, 3)).reshape(token_count, local_heads * HEAD_DIM)
    attended = attended.astype(jnp.bfloat16)
    projected = jnp.dot(
        lax.all_gather(attended, "tp", axis=1, tiled=True),
        out_weight,
        preferred_element_type=jnp.float32,
    )
    mixed_sum = residual.astype(jnp.float32) + projected
    mixed_rows = mixed_sum.astype(jnp.bfloat16)
    full_rows = lax.all_gather(mixed_rows, "tp", axis=1, tiled=True)
    width_total = full_rows.shape[1]
    per_sp = tp_size // 2
    column = tp_place // 2
    experts_total = per_sp * sp_size
    capacity = 3 * token_count * TOP_K // (2 * experts_total)
    slot_count = sp_size * capacity
    flat_choice = route_expert.reshape(token_count * TOP_K)
    onehot = (flat_choice[:, None] == jnp.arange(experts_total, dtype=jnp.int32)[None, :]).astype(
        jnp.int32
    )
    earlier = jnp.cumsum(onehot, axis=0) - onehot
    slot_rank = jnp.sum(earlier * onehot, axis=1)
    mine = flat_choice % per_sp == column
    target = flat_choice // per_sp * capacity + slot_rank
    owner = jnp.arange(token_count * TOP_K, dtype=jnp.int32) // TOP_K
    slot_token = (
        jnp.full((slot_count + 1,), token_count, jnp.int32)
        .at[jnp.where(mine, target, slot_count)]
        .set(owner)[:slot_count]
    )
    padded = jnp.concatenate([full_rows, jnp.zeros((1, width_total), jnp.bfloat16)], axis=0)
    selected = padded[slot_token].reshape(sp_size, capacity, width_total)
    arrived = lax.all_to_all(selected, "sp", split_axis=0, concat_axis=0, tiled=True)
    expert_rows = arrived.reshape(slot_count, width_total)
    squares = jnp.mean(jnp.square(expert_rows.astype(jnp.float32)), axis=-1, keepdims=True)
    norm_scale = lax.rsqrt(squares + EPSILON)
    gate_value = (
        jnp.dot(expert_rows, expert_gate[0], preferred_element_type=jnp.float32) * norm_scale
    )
    up_value = jnp.dot(expert_rows, expert_up[0], preferred_element_type=jnp.float32) * norm_scale
    hidden = (jax.nn.silu(gate_value) * up_value).astype(jnp.bfloat16)
    half_result = jnp.dot(hidden, expert_down[0], preferred_element_type=jnp.float32).astype(
        jnp.bfloat16
    )
    returned = lax.all_to_all(
        half_result.reshape(sp_size, capacity, width_total),
        "sp",
        split_axis=0,
        concat_axis=0,
        tiled=True,
    )
    slot_results = returned.reshape(slot_count, width_total)
    mine_grid = mine.reshape(token_count, TOP_K)
    target_grid = target.reshape(token_count, TOP_K)
    gathered_sum = jnp.zeros((token_count, width_total), jnp.float32)
    for choice_index in range(TOP_K):
        chosen = mine_grid[:, choice_index]
        index = jnp.where(chosen, target_grid[:, choice_index], 0)
        factor = jnp.where(chosen, route_weight[:, choice_index], 0.0)
        picked = slot_results[index].astype(jnp.float32)
        gathered_sum = gathered_sum + factor[:, None] * picked
    routed = lax.psum_scatter(
        gathered_sum.astype(jnp.bfloat16), "tp", scatter_dimension=1, tiled=True
    ).astype(jnp.float32)
    return (mixed_sum + routed).astype(jnp.bfloat16)


def normed_heads(proj, gain, cosine_table, sine_table):
    token_count = proj.shape[0]
    heads = proj.reshape(token_count, gain.shape[0], HEAD_DIM)
    return rotate(head_norm(heads, gain), cosine_table, sine_table).astype(jnp.bfloat16)


def flip(value, axis, mask):
    return lax.ppermute(value, axis, [(i, i ^ mask) for i in range(lax.axis_size(axis))])


def add_rounded(mine, other):
    return (mine.astype(jnp.float32) + other.astype(jnp.float32)).astype(jnp.bfloat16)


def relative_blocks(weight, place, axis):
    width = weight.shape[axis] // 4
    return jnp.concatenate(
        [lax.dynamic_slice_in_dim(weight, (place ^ q) * width, width, axis) for q in range(4)],
        axis=axis,
    )


def flip_index(index, mask):
    bit = 1
    while bit <= mask:
        if mask & bit:
            index = index + bit - 2 * bit * ((index // bit) % 2)
        bit *= 2
    return index


KINDS = 16
Z_OUT, X_ONE, Y_ONE, X_TWO, Y_TWO, CORE_OUT, CORE_BACK, X_SUM = range(8)
Y_SUM, Y_PASS, X_PASS, Z_BACK, X_HEADS, Y_HEADS, X_MORE, Y_MORE = range(8, KINDS)


def experts_kernel(
    chips,
    heads_ref,
    residual_ref,
    out_weight_ref,
    gate_up_ref,
    down_ref,
    factor_ref,
    out_ref,
    heads,
    x_ref,
    rows,
    outs,
    core_in,
    send_x,
    send_y,
    got_x,
    got_y,
    pass_y,
    pass_x,
    end_y,
    end_x,
    send_z,
    got_z,
    send_sem,
    recv_sem,
):
    sp_place, tp_place = lax.axis_index("sp"), lax.axis_index("tp")
    over_x = {"tp": flip_index(tp_place, 1)}
    over_y = {"tp": flip_index(tp_place, 2)}
    core = {"sp": flip_index(sp_place, 1)}
    over_z = [{"sp": flip_index(sp_place, 2 * d)} for d in range(1, chips)]
    f32, bf16 = jnp.float32, jnp.bfloat16
    count, width = heads_ref.shape
    half = count // 2
    hidden_units = down_ref.shape[0]
    upper, lower = pl.ds(0, half), pl.ds(half, half)

    def quarter(q):
        return pl.ds(q * width, width)

    barrier = pltpu.get_barrier_semaphore()
    partners = [over_x, over_y, core] + over_z
    for partner in partners:
        pl.semaphore_signal(
            barrier, inc=1, device_id=partner, device_id_type=pl.DeviceIdType.MESH
        )
    pl.semaphore_wait(barrier, len(partners))

    copies, waited = {}, []

    def send(kind, d, src, dst, device):
        copies[kind, d] = pltpu.make_async_remote_copy(
            src_ref=src,
            dst_ref=dst,
            send_sem=send_sem.at[kind, d],
            recv_sem=recv_sem.at[kind, d],
            device_id=device,
            device_id_type=pl.DeviceIdType.MESH,
        )
        copies[kind, d].start()

    def arrived(kind, d):
        copies[kind, d].wait_recv()

    def spread(d):
        if d and d not in waited:
            arrived(Z_OUT, d)
        if d:
            block = rows.at[d, 0, :, quarter(0)]
        else:
            block = x_ref
        send(X_ONE, d, block, rows.at[d, 0, :, quarter(1)], over_x)
        send(Y_ONE, d, block, rows.at[d, 0, :, quarter(2)], over_y)

    def spread_on(d):
        arrived(Y_ONE, d)
        send(X_TWO, d, rows.at[d, 0, upper, quarter(2)], rows.at[d, 0, upper, quarter(3)], over_x)
        arrived(X_ONE, d)
        send(Y_TWO, d, rows.at[d, 0, lower, quarter(1)], rows.at[d, 0, lower, quarter(3)], over_y)

    def swap_cores(d):
        arrived(X_TWO, d)
        arrived(Y_TWO, d)
        send(CORE_OUT, d, rows.at[d, 0], rows.at[d, 1], core)

    def compute(d):
        arrived(CORE_OUT, d)

        def one(i, carry):
            side = 1 - i
            own_rows = rows[d, side]
            wide = own_rows.astype(f32)
            squares = jnp.mean(wide * wide, axis=-1, keepdims=True)
            norm_scale = lax.rsqrt(squares + EPSILON)
            both = jnp.dot(own_rows, gate_up_ref[...], preferred_element_type=f32) * norm_scale
            gate_value, up_value = both[:, :hidden_units], both[:, hidden_units:]
            hidden = (gate_value / (1.0 + jnp.exp(-gate_value)) * up_value).astype(bf16)
            factor = factor_ref[d, side]
            for q in range(4):
                part = jnp.dot(hidden, down_ref[:, quarter(q)], preferred_element_type=f32)
                outs[d, side, :, quarter(q)] = (part.astype(bf16).astype(f32) * factor).astype(bf16)
            return carry

        lax.fori_loop(0, 2, one, 0)
        send(CORE_BACK, d, outs.at[d, 1], core_in.at[d], core)

    def both_cores(d, span, q):
        mine = outs[d, 0, span, quarter(q)].astype(f32)
        return (mine + core_in[d, span, quarter(q)].astype(f32)).astype(bf16)

    def gather_sums(d):
        arrived(CORE_BACK, d)
        send_x[d, :, quarter(0)] = both_cores(d, upper, 1)
        send_x[d, :, quarter(1)] = both_cores(d, upper, 3)
        send(X_SUM, d, send_x.at[d], got_x.at[d], over_x)
        send_y[d, :, quarter(0)] = both_cores(d, lower, 2)
        send_y[d, :, quarter(1)] = both_cores(d, lower, 3)
        send(Y_SUM, d, send_y.at[d], got_y.at[d], over_y)

    def pass_sums(d):
        arrived(X_SUM, d)
        pass_y[d] = add_rounded(both_cores(d, upper, 2), got_x[d, :, quarter(1)])
        send(Y_PASS, d, pass_y.at[d], end_y.at[d], over_y)
        arrived(Y_SUM, d)
        pass_x[d] = add_rounded(both_cores(d, lower, 1), got_y[d, :, quarter(1)])
        send(X_PASS, d, pass_x.at[d], end_x.at[d], over_x)

    def finish(d):
        arrived(Y_PASS, d)
        top = both_cores(d, upper, 0).astype(f32) + got_x[d, :, quarter(0)].astype(f32)
        top = top + end_y[d].astype(f32)
        arrived(X_PASS, d)
        bottom = both_cores(d, lower, 0).astype(f32) + got_y[d, :, quarter(0)].astype(f32)
        bottom = bottom + end_x[d].astype(f32)
        if d:
            send_z[d, upper, :] = top.astype(bf16)
            send_z[d, lower, :] = bottom.astype(bf16)
            send(Z_BACK, d, send_z.at[d], got_z.at[d], over_z[d - 1])
        else:
            out_ref[upper, :] += top
            out_ref[lower, :] += bottom

    def send_rows(d):
        send(Z_OUT, d, x_ref, rows.at[d, 0, :, quarter(0)], over_z[d - 1])

    def send_rows_after(d):
        waited.append(d - 1)
        arrived(Z_OUT, d - 1)
        send_rows(d)

    send(X_HEADS, 0, heads_ref, heads.at[:, quarter(1)], over_x)
    send(Y_HEADS, 0, heads_ref, heads.at[:, quarter(2)], over_y)
    projected = jnp.dot(heads_ref[...], out_weight_ref[quarter(0), :], preferred_element_type=f32)
    projected = projected + residual_ref[...].astype(f32)
    arrived(Y_HEADS, 0)
    send(X_MORE, 0, heads.at[upper, quarter(2)], heads.at[upper, quarter(3)], over_x)
    arrived(X_HEADS, 0)
    send(Y_MORE, 0, heads.at[lower, quarter(1)], heads.at[lower, quarter(3)], over_y)
    for q in (1, 2):
        projected = projected + jnp.dot(
            heads[:, quarter(q)], out_weight_ref[quarter(q), :], preferred_element_type=f32
        )
    arrived(X_MORE, 0)
    arrived(Y_MORE, 0)
    projected = projected + jnp.dot(
        heads[:, quarter(3)], out_weight_ref[quarter(3), :], preferred_element_type=f32
    )
    x_ref[...] = projected.astype(bf16)
    rows[0, 0, :, quarter(0)] = projected.astype(bf16)
    out_ref[...] = projected

    if chips == 4:
        schedule = (
            [(send_rows, 1), (send_rows, 2), (spread, 0), (spread, 1), (spread_on, 0)]
            + [(swap_cores, 0), (compute, 0), (send_rows_after, 3), (spread, 2)]
            + [(spread_on, 1), (swap_cores, 1), (compute, 1), (gather_sums, 1), (spread, 3)]
            + [(spread_on, 2), (pass_sums, 1), (swap_cores, 2), (compute, 2)]
            + [(gather_sums, 2), (spread_on, 3), (finish, 1), (pass_sums, 2), (swap_cores, 3)]
            + [(compute, 3), (gather_sums, 3), (finish, 2), (gather_sums, 0), (pass_sums, 3)]
            + [(finish, 3), (pass_sums, 0), (finish, 0)]
        )
    else:
        schedule = [(send_rows, d) for d in range(1, chips)]
        stages = (spread, spread_on, swap_cores, compute, gather_sums, pass_sums, finish)
        for step in range(chips + len(stages) - 1):
            for delay, stage in enumerate(stages):
                if 0 <= step - delay < chips:
                    schedule.append((stage, step - delay))
    for stage, d in schedule:
        stage(d)
    for d in range(1, chips):
        arrived(Z_BACK, d)
        out_ref[...] += got_z[d].astype(f32)
    for copy in copies.values():
        copy.wait_send()


def project_and_experts(attended, residual, out_weight, gate_up, down, factors):
    chips = factors.shape[0]
    count, width = attended.shape
    half, total = count // 2, down.shape[1]
    bf16 = jnp.bfloat16
    shapes = [
        (count, total),
        (count, width),
        (chips, 2, count, total),
        (chips, 2, count, total),
        (chips, count, total),
        (chips, half, 2 * width),
        (chips, half, 2 * width),
        (chips, half, 2 * width),
        (chips, half, 2 * width),
        (chips, half, width),
        (chips, half, width),
        (chips, half, width),
        (chips, half, width),
        (chips, count, width),
        (chips, count, width),
    ]
    sems = pltpu.SemaphoreType.DMA((KINDS, chips))
    return pl.pallas_call(
        functools.partial(experts_kernel, chips),
        out_shape=jax.ShapeDtypeStruct((count, width), jnp.float32),
        in_specs=[pl.BlockSpec(memory_space=pltpu.VMEM)] * 6,
        out_specs=pl.BlockSpec(memory_space=pltpu.VMEM),
        scratch_shapes=[pltpu.VMEM(shape, bf16) for shape in shapes] + [sems, sems],
        compiler_params=pltpu.CompilerParams(
            collective_id=0, has_side_effects=True, vmem_limit_bytes=52 * 1024 * 1024
        ),
    )(attended, residual, out_weight, gate_up, down, factors)


def local_dense(
    query_proj,
    key_proj,
    value_proj,
    query_gain,
    key_gain,
    residual,
    out_weight,
    route_expert,
    route_weight,
    expert_gate,
    expert_up,
    expert_down,
):
    token_count = query_proj.shape[0]
    local_heads = query_gain.shape[0]
    local_kv = key_gain.shape[0]
    group_size = local_heads // local_kv
    sp_size = lax.axis_size("sp")
    tp_size = lax.axis_size("tp")
    sp_place = lax.axis_index("sp")
    tp_place = lax.axis_index("tp")
    chips = sp_size // 2
    experts_total = sp_size * tp_size // 2
    my_expert = (sp_place * tp_size + tp_place) // 2
    cosine_table, sine_table = rotation_tables(sp_place * token_count, token_count)

    key_rot = normed_heads(key_proj, key_gain, cosine_table, sine_table)
    packed = jnp.concatenate(
        [key_rot.reshape(token_count, local_kv * HEAD_DIM), value_proj], axis=1
    )
    kv_blocks = [packed] + [flip(packed, "sp", 2 * d) for d in range(1, chips)]

    ids = jnp.arange(experts_total, dtype=jnp.int32)
    chosen = route_expert.T[None, :, :] == ids[:, None, None]
    table = jnp.sum(jnp.where(chosen, route_weight.T[None, :, :], 0.0), axis=1)
    tables = jnp.stack([table] + [flip(table, "sp", 2 * d) for d in range(1, chips)])
    tables = jnp.stack([tables, flip(tables, "sp", 1)])
    factors = jnp.sum(jnp.where(ids[:, None] == my_expert, tables, 0.0), axis=2)

    query_rot = normed_heads(query_proj, query_gain, cosine_table, sine_table)
    query_groups = query_rot.reshape(token_count, local_kv, group_size, HEAD_DIM)
    running = (
        jnp.full((local_kv, group_size, token_count), -1e30, jnp.float32),
        jnp.zeros((local_kv, group_size, token_count), jnp.float32),
        jnp.zeros((local_kv, group_size, token_count, HEAD_DIM), jnp.float32),
    )
    for block in kv_blocks:
        both = jnp.concatenate([block, flip(block, "sp", 1)], axis=0)
        key_block = both[:, : local_kv * HEAD_DIM].reshape(-1, local_kv, HEAD_DIM)
        value_block = both[:, local_kv * HEAD_DIM :].reshape(-1, local_kv, HEAD_DIM)
        running = online_update(running, query_groups, key_block, value_block)
    final_max, final_sum, final_acc = running
    attended = final_acc / final_sum[..., None]
    attended = jnp.transpose(attended, (2, 0, 1, 3)).reshape(token_count, local_heads * HEAD_DIM)
    attended = attended.astype(jnp.bfloat16)

    out_relative = relative_blocks(out_weight, tp_place, 0)
    gate_up = relative_blocks(
        jnp.concatenate([expert_gate[0], expert_up[0]], axis=1), tp_place, 0
    )
    down = relative_blocks(expert_down[0], tp_place, 1)
    hidden_units = expert_down.shape[1]

    columns = jnp.transpose(factors, (1, 0, 2))[..., None]
    result = project_and_experts(attended, residual, out_relative, gate_up, down, columns)
    return result.astype(jnp.bfloat16)


def takes_dense(mesh):
    chips = mesh.shape["sp"] // 2
    experts_total = mesh.shape["sp"] * mesh.shape["tp"] // 2
    power = mesh.shape["sp"] % 2 == 0 and chips & (chips - 1) == 0
    return mesh.shape["tp"] == 4 and power and experts_total <= 2 * TOP_K


def solution(mesh):
    in_specs = (
        P("sp", "tp"),
        P("sp", "tp"),
        P("sp", "tp"),
        P("tp", None),
        P("tp", None),
        P("sp", "tp"),
        P(None, "tp"),
        P("sp", None),
        P("sp", None),
        P(("sp", "tp"), None, None),
        P(("sp", "tp"), None, None),
        P(("sp", "tp"), None, None),
    )
    out_specs = P("sp", "tp")
    body = local_dense if takes_dense(mesh) else local
    return jax.shard_map(body, mesh=mesh, in_specs=in_specs, out_specs=out_specs, check_vma=False)
```
